512 devices in a mesh: sp: 64 (over z, y), dp: 8 (over x, core).
Axes of the slice: x: 4, y: 4, z: 16, core: 2. Of those that a mesh axis runs over, the one named last changes fastest.
Arguments:
- val_input: bfloat16 [8192, 1536], P('sp', 'dp'), may hold values from -24 to 24, as said below
- gate_input: bfloat16 [8192, 1536], P('sp', 'dp'), may hold values from -8 to 8
- cotangent: bfloat16 [8192, 4096], P('sp'), may hold values from -16 to 16
- out_weight: bfloat16 [4096, 1536], P('sp', 'dp'), may hold values from -0.09375 to 0.09375
- conv_taps: float32 [31, 1536], P(None, 'dp'), may hold values from -1 to 1
- norm_gain: float32 [1536], P('dp'), may hold values from 0.1 to 1.9
Outputs:
- grad_val: bfloat16 [8192, 1536], P('sp', 'dp')
- grad_gate: bfloat16 [8192, 1536], P('sp', 'dp')
- grad_out_weight: float32 [4096, 1536], P('sp', 'dp')
- grad_taps: float32 [31, 1536], P(None, 'dp')
- grad_gain: float32 [1536], P('dp')
The draws below stay inside these ranges and needn't reach their ends.
Inputs may be any that keep to these rules, and one draw needn't show every extreme that they name: `val_input`: blocks of 64 channels and blocks of 32 tokens carry their own scales.
All inputs are finite; a program needn't handle non-finite values.
Results may differ from the reference program's by a relative error of at most 0.0063.
Values may be sent and summed in bfloat16 or wider, within the bound.
No kernel may reach another device: no remote copies, remote signals or barrier semaphores. Data moves between devices by JAX's collectives and lax.ppermute only.
A program may use at most 64 MiB of HBM per device.

```python
import jax
import jax.numpy as jnp
from jax import lax

D = 4096
C = 1536
KERNEL = 31
TOKENS = 8192


def draw_val_input(key, part):
    first, second, third = jax.random.split(key, 3)
    base = jax.random.normal(first, (TOKENS, C), jnp.float32)
    block_scale = jnp.exp(jax.random.uniform(second, (C // 64,), jnp.float32, jnp.log(0.3), jnp.log(3.0)))
    time_scale = jnp.exp(jax.random.uniform(third, (TOKENS // 32,), jnp.float32, jnp.log(0.5), jnp.log(2.0)))
    values = base * jnp.repeat(block_scale, 64)[None, :] * jnp.repeat(time_scale, 32)[:, None]
    return jnp.clip(values, -24.0, 24.0).astype(jnp.bfloat16)


def with_spikes(values, rng, source, target, blocks, factor):
    owner, partner = [(jnp.arange(values.shape[position]) // (values.shape[position] // blocks)).reshape([-1 if axis == position else 1 for axis in range(values.ndim)]) for position in (source, target)]
    chosen = jax.random.permutation(rng, blocks)[partner]
    strong = (owner == chosen) | (owner == (partner + blocks // 2) % blocks)
    return jnp.where(strong, factor * values, values)


def shard_levels(own_key, dims, pieces, low, top_value):
    def one(dim, parts):
        draws = jax.random.uniform(jax.random.fold_in(jax.random.fold_in(own_key, 6), dim), (parts,), jnp.float32, low / len(pieces), top_value / len(pieces))
        return jnp.repeat(jnp.exp(draws), dims[dim] // parts).reshape((-1,) + (1,) * (len(dims) - dim - 1))

    factor_of = one(*pieces[0])
    for cut in pieces[1:]:
        factor_of = factor_of * one(*cut)
    return factor_of


def bell_draw(key, shape, scale, bound, shards=(), held_as=jnp.bfloat16):
    entries = scale * jax.random.normal(key, shape, jnp.float32)
    if shards:
        entries = entries * shard_levels(key, shape, shards, -0.22, 0.18)
    return jnp.clip(entries, -bound, bound).astype(held_as)


def gaussian_with(key, extent, scale, limit, pieces, heavy, kind=jnp.bfloat16):
    entries = scale * jax.random.normal(key, extent, jnp.float32)
    if pieces:
        entries = entries * shard_levels(key, extent, pieces, -0.22, 0.18)
    return jnp.clip(with_spikes(entries, jax.random.fold_in(key, 3), *heavy), -limit, limit).astype(kind)


def setup_inputs(seed: int = 0) -> dict:
    keys = jax.random.split(jax.random.key(seed), 7)
    return {
        "val_input": draw_val_input(jax.random.fold_in(keys[6], 71), 0),
        "gate_input": bell_draw(keys[1], (TOKENS, C), 1.5, 8.0, ((0, 64), (1, 8))),
        "cotangent": gaussian_with(keys[2], (TOKENS, D), 1.0, 16.0, ((0, 64),), (0, 1, 64, 4.0)),
        "out_weight": bell_draw(keys[3], (D, C), D ** -0.5, 0.09375, ((0, 64), (1, 8))),
        "conv_taps": bell_draw(keys[4], (KERNEL, C), KERNEL ** -0.5, 1.0, ((1, 8),), jnp.float32),
        "norm_gain": jnp.clip(1.0 + 0.18 * jax.random.normal(keys[5], (C,), jnp.float32), 0.1, 1.9),
    }


norm_floor = 0.25

def reference(val_input, gate_input, cotangent, out_weight, conv_taps, norm_gain):
    length = val_input.shape[0]
    sigma_gate = jax.nn.sigmoid(gate_input.astype(jnp.float32))
    mixed_in = (val_input.astype(jnp.float32) * sigma_gate).astype(jnp.bfloat16)
    padded_in = jnp.pad(lax.optimization_barrier(mixed_in).astype(jnp.float32), ((KERNEL - 1, 0), (0, 0)))
    conv_out = jnp.zeros((length, C), jnp.float32)
    for offset in range(KERNEL):
        conv_out = conv_out + conv_taps[offset][None, :] * padded_in[offset:offset + length]
    conv_rows = lax.optimization_barrier(conv_out.astype(jnp.bfloat16)).astype(jnp.float32)
    row_mean = lax.optimization_barrier(jnp.sum(conv_rows, 1, keepdims=True)) / C
    row_var = lax.optimization_barrier(jnp.sum(conv_rows * conv_rows, 1, keepdims=True)) / C - row_mean * row_mean
    inv_scale = lax.rsqrt(row_var + norm_floor)
    normed = (conv_rows - row_mean) * inv_scale
    act = normed * norm_gain[None, :]
    sigma_act = jax.nn.sigmoid(act)
    swished = (act * sigma_act).astype(jnp.bfloat16)
    grad_mix = jnp.dot(cotangent, out_weight, preferred_element_type=jnp.float32)
    grad_out_weight = lax.dot_general(cotangent, swished, (((0,), (0,)), ((), ())), preferred_element_type=jnp.float32)
    grad_act = grad_mix * sigma_act * (1.0 + act * (1.0 - sigma_act))
    grad_gain = lax.optimization_barrier(jnp.sum(grad_act * normed, 0))
    grad_norm = grad_act * norm_gain[None, :]
    first_sum = lax.optimization_barrier(jnp.sum(grad_norm, 1, keepdims=True)) / C
    second_sum = lax.optimization_barrier(jnp.sum(grad_norm * normed, 1, keepdims=True)) / C
    grad_conv = (inv_scale * (grad_norm - first_sum - normed * second_sum)).astype(jnp.bfloat16)
    grad_float = lax.optimization_barrier(grad_conv).astype(jnp.float32)
    padded_grad = jnp.pad(grad_float, ((0, KERNEL - 1), (0, 0)))
    grad_mixed = jnp.zeros((length, C), jnp.float32)
    tap_list = []
    for offset in range(KERNEL):
        back = KERNEL - 1 - offset
        grad_mixed = grad_mixed + conv_taps[offset][None, :] * padded_grad[back:back + length]
        tap_list.append(lax.optimization_barrier(jnp.sum(grad_float * padded_in[offset:offset + length], 0)))
    grad_taps = jnp.stack(tap_list, 0)
    grad_rows = lax.optimization_barrier(grad_mixed.astype(jnp.bfloat16)).astype(jnp.float32)
    grad_val = (grad_rows * sigma_gate).astype(jnp.bfloat16)
    grad_gate = (grad_rows * val_input.astype(jnp.float32) * sigma_gate * (1.0 - sigma_gate)).astype(jnp.bfloat16)
    return (grad_val, grad_gate, grad_out_weight, grad_taps, grad_gain)
```

```python
import jax
import jax.numpy as jnp
from jax import lax
from jax.sharding import Mesh
from jax.sharding import PartitionSpec as P

SP = ("sp_0", "sp_1")


norm_floor = 0.25


def passed_along(value, axis, steps):
    count = lax.axis_size(axis)
    first, last = (max(0, -steps), min(count, count - steps))
    return lax.ppermute(value, axis, [(source, source + steps) for source in range(first, last)])


def exchange(blocks, axis):
    return lax.all_to_all(blocks, axis, split_axis=0, concat_axis=0, tiled=True)


def from_everyone(array, axis):
    return exchange(jnp.broadcast_to(array, (lax.axis_size(axis), *array.shape)), axis)


def packed_total(arrays, axis):
    ravelled = jnp.concatenate([a.reshape(-1) for a in arrays])
    total = from_everyone(ravelled, axis).sum(axis=0)
    at, finished = 0, []
    for a in arrays:
        finished.append(total[at : at + a.size].reshape(a.shape))
        at += a.size
    return tuple(finished)


def dense(blocks):
    half = blocks.shape[-2] // 2
    rest = jnp.concatenate([blocks[..., :half, 128:], blocks[..., half:, 128:]], -1)
    return jnp.concatenate([blocks[..., :128], rest], -2)


def undense(blocks):
    rows = blocks.shape[-2] * 2 // 3
    rest = blocks[..., rows:, :]
    rest = jnp.concatenate([rest[..., :64], rest[..., 64:]], -2)
    return jnp.concatenate([blocks[..., :rows, :], rest], -1)


def per_device(val_input, gate_input, cotangent, out_weight, conv_taps, norm_gain):
    rows_here = val_input.shape[0]
    width_dp = val_input.shape[1]
    taps = conv_taps.shape[0]
    channels = width_dp * lax.axis_size("dp")
    z_size, y_size = (lax.axis_size("sp_0"), lax.axis_size("sp_1"))
    d_rows = out_weight.shape[0]

    weight = undense(from_everyone(dense(out_weight), "sp_0")).reshape(z_size * d_rows, width_dp)
    columns = cotangent.reshape(rows_here, z_size, y_size, d_rows).transpose(2, 0, 1, 3)
    columns = exchange(columns.reshape(y_size, rows_here, z_size * d_rows), "sp_1")
    columns = columns.reshape(y_size * rows_here, z_size * d_rows)

    sigma_gate = jax.nn.sigmoid(gate_input.astype(jnp.float32))
    mixed_in = (val_input.astype(jnp.float32) * sigma_gate).astype(jnp.bfloat16)
    earlier = passed_along(mixed_in[rows_here - (taps - 1) :], SP, 1)
    padded_in = jnp.concatenate([earlier, lax.optimization_barrier(mixed_in)], 0).astype(
        jnp.float32
    )
    conv_out = jnp.zeros((rows_here, width_dp), jnp.float32)
    for offset in range(taps):
        conv_out = conv_out + conv_taps[offset][None, :] * padded_in[offset : offset + rows_here]
    conv_rows = lax.optimization_barrier(conv_out.astype(jnp.bfloat16)).astype(jnp.float32)
    row_sums = packed_total((jnp.sum(conv_rows, 1), jnp.sum(conv_rows * conv_rows, 1)), "dp")
    row_mean = row_sums[0][:, None] / channels
    row_var = row_sums[1][:, None] / channels - row_mean * row_mean
    inv_scale = lax.rsqrt(row_var + norm_floor)
    normed = (conv_rows - row_mean) * inv_scale
    act = normed * norm_gain[None, :]
    sigma_act = jax.nn.sigmoid(act)
    swished = (act * sigma_act).astype(jnp.bfloat16)

    swished_y = from_everyone(swished, "sp_1").reshape(y_size * rows_here, width_dp)
    weight_part = lax.dot_general(
        columns, swished_y, (((0,), (0,)), ((), ())), preferred_element_type=jnp.float32
    )
    weight_part = weight_part.astype(jnp.bfloat16).reshape(z_size, d_rows, width_dp)
    weight_part = exchange(dense(weight_part), "sp_0").astype(jnp.float32)
    grad_out_weight = undense(weight_part.sum(axis=0))

    mix_part = jnp.dot(columns, weight, preferred_element_type=jnp.float32).astype(jnp.bfloat16)
    mix_part = exchange(mix_part.reshape(y_size, rows_here, width_dp), "sp_1")
    grad_mix = mix_part.astype(jnp.float32).sum(axis=0)

    grad_act = grad_mix * sigma_act * (1.0 + act * (1.0 - sigma_act))
    gain_part = jnp.sum(grad_act * normed, 0)
    grad_norm = grad_act * norm_gain[None, :]
    norm_sums = packed_total((jnp.sum(grad_norm, 1), jnp.sum(grad_norm * normed, 1)), "dp")
    first_sum = norm_sums[0][:, None] / channels
    second_sum = norm_sums[1][:, None] / channels
    grad_conv = (inv_scale * (grad_norm - first_sum - normed * second_sum)).astype(jnp.bfloat16)
    grad_conv = lax.optimization_barrier(grad_conv)
    own_grad = grad_conv.astype(jnp.float32)
    tap_list = []
    for offset in range(taps):
        tap_list.append(jnp.sum(own_grad * padded_in[offset : offset + rows_here], 0))
    tail = jnp.stack(tap_list + [gain_part], 0)
    tail = tail.reshape(y_size, (taps + 1) // y_size, width_dp)
    tail = exchange(tail, "sp_1").sum(axis=0).astype(jnp.bfloat16)
    tail = from_everyone(tail, "sp_0").astype(jnp.float32).sum(axis=0)
    tail = from_everyone(tail, "sp_1").reshape(taps + 1, width_dp)
    grad_taps, grad_gain = (tail[:taps], tail[taps])

    later = passed_along(grad_conv[: taps - 1], SP, -1)
    padded_grad = jnp.concatenate([grad_conv, later], 0).astype(jnp.float32)
    grad_mixed = jnp.zeros((rows_here, width_dp), jnp.float32)
    for offset in range(taps):
        back = taps - 1 - offset
        grad_mixed = grad_mixed + conv_taps[offset][None, :] * padded_grad[back : back + rows_here]
    grad_rows = lax.optimization_barrier(grad_mixed.astype(jnp.bfloat16)).astype(jnp.float32)
    grad_val = (grad_rows * sigma_gate).astype(jnp.bfloat16)
    grad_gate = (
        grad_rows * val_input.astype(jnp.float32) * sigma_gate * (1.0 - sigma_gate)
    ).astype(jnp.bfloat16)
    return (grad_val, grad_gate, grad_out_weight, grad_taps, grad_gain)


def solution(mesh):
    split = Mesh(mesh.devices.reshape(16, 4, mesh.shape["dp"]), ("sp_0", "sp_1", "dp"))
    in_specs = (P(SP, "dp"), P(SP, "dp"), P(SP, None), P(SP, "dp"), P(None, "dp"), P("dp"))
    out_specs = (P(SP, "dp"), P(SP, "dp"), P(SP, "dp"), P(None, "dp"), P("dp"))
    return jax.shard_map(
        per_device, mesh=split, in_specs=in_specs, out_specs=out_specs, check_vma=False
    )
```

```python
import jax
import jax.numpy as jnp
from jax import lax
from jax.sharding import Mesh
from jax.sharding import PartitionSpec as P


SP = ("sp_0", "sp_1")


norm_floor = 0.25


def passed_along(value, axis, steps):
    count = lax.axis_size(axis)
    first, last = (max(0, -steps), min(count, count - steps))
    return lax.ppermute(value, axis, [(source, source + steps) for source in range(first, last)])


def exchange(blocks, axis):
    return lax.all_to_all(blocks, axis, split_axis=0, concat_axis=0, tiled=True)


def from_everyone(array, axis):
    return exchange(jnp.broadcast_to(array, (lax.axis_size(axis), *array.shape)), axis)


def shifted(value, axis, steps):
    count = lax.axis_size(axis)
    return lax.ppermute(value, axis, [(i, (i + steps) % count) for i in range(count)])


def chip_pairs_total(value, axis):
    count = lax.axis_size(axis)
    value = value + lax.ppermute(value, axis, [(i, i ^ 1) for i in range(count)])
    others = [shifted(value, axis, k) for k in range(2, count, 2)]
    return sum(others, value)


def dense(blocks):
    half = blocks.shape[-2] // 2
    rest = jnp.concatenate([blocks[..., :half, 128:], blocks[..., half:, 128:]], -1)
    return jnp.concatenate([blocks[..., :128], rest], -2)


def undense(blocks):
    rows = blocks.shape[-2] * 2 // 3
    rest = blocks[..., rows:, :]
    rest = jnp.concatenate([rest[..., :64], rest[..., 64:]], -2)
    return jnp.concatenate([blocks[..., :rows, :], rest], -1)


def per_device(val_input, gate_input, cotangent, out_weight, conv_taps, norm_gain):
    rows_here = val_input.shape[0]
    width_dp = val_input.shape[1]
    taps = conv_taps.shape[0]
    channels = width_dp * lax.axis_size("dp")
    z_size, y_size = (lax.axis_size("sp_0"), lax.axis_size("sp_1"))
    d_rows = out_weight.shape[0]

    y_here = lax.axis_index("sp_1")
    ahead = range(1, y_size)

    weight = from_everyone(dense(out_weight), "sp_0")
    blocks = cotangent.reshape(rows_here, z_size, y_size, d_rows).transpose(2, 0, 1, 3)
    blocks = blocks.reshape(y_size, rows_here, z_size * d_rows)
    blocks = [lax.dynamic_index_in_dim(blocks, (y_here + k) % y_size, 0, False) for k in range(y_size)]
    columns = [blocks[0]] + [shifted(blocks[k], "sp_1", k) for k in ahead]

    sigma_gate = jax.nn.sigmoid(gate_input.astype(jnp.float32))
    mixed_in = (val_input.astype(jnp.float32) * sigma_gate).astype(jnp.bfloat16)
    earlier = passed_along(mixed_in[rows_here - (taps - 1) :], SP, 1)
    padded_in = jnp.concatenate([earlier, lax.optimization_barrier(mixed_in)], 0).astype(
        jnp.float32
    )
    conv_out = jnp.zeros((rows_here, width_dp), jnp.float32)
    for offset in range(taps):
        conv_out = conv_out + conv_taps[offset][None, :] * padded_in[offset : offset + rows_here]
    conv_rows = lax.optimization_barrier(conv_out.astype(jnp.bfloat16)).astype(jnp.float32)
    row_sums = jnp.stack([jnp.sum(conv_rows, 1), jnp.sum(conv_rows * conv_rows, 1)])
    row_sums = chip_pairs_total(row_sums, "dp")
    row_mean = row_sums[0][:, None] / channels
    row_var = row_sums[1][:, None] / channels - row_mean * row_mean
    inv_scale = lax.rsqrt(row_var + norm_floor)
    normed = (conv_rows - row_mean) * inv_scale
    act = normed * norm_gain[None, :]
    sigma_act = jax.nn.sigmoid(act)
    swished = (act * sigma_act).astype(jnp.bfloat16)

    swished_y = jnp.concatenate([swished] + [shifted(swished, "sp_1", k) for k in ahead], 0)
    weight_part = lax.dot_general(
        jnp.concatenate(columns, 0),
        swished_y,
        (((0,), (0,)), ((), ())),
        preferred_element_type=jnp.float32,
    )
    weight_part = weight_part.astype(jnp.bfloat16).reshape(z_size, d_rows, width_dp)
    weight, weight_part = lax.optimization_barrier((weight, dense(weight_part)))
    weight = undense(weight).reshape(z_size * d_rows, width_dp)
    weight_part = exchange(weight_part, "sp_0")

    mix_parts = [
        jnp.dot(c, weight, preferred_element_type=jnp.float32).astype(jnp.bfloat16) for c in columns
    ]
    mix_parts = [mix_parts[0]] + [shifted(mix_parts[k], "sp_1", -k) for k in ahead]
    grad_mix = sum(p.astype(jnp.float32) for p in mix_parts)

    grad_act = grad_mix * sigma_act * (1.0 + act * (1.0 - sigma_act))
    gain_part = jnp.sum(grad_act * normed, 0)
    grad_norm = grad_act * norm_gain[None, :]
    norm_sums = jnp.stack([jnp.sum(grad_norm, 1), jnp.sum(grad_norm * normed, 1)])
    norm_sums = chip_pairs_total(norm_sums, "dp")
    first_sum = norm_sums[0][:, None] / channels
    second_sum = norm_sums[1][:, None] / channels
    grad_conv = (inv_scale * (grad_norm - first_sum - normed * second_sum)).astype(jnp.bfloat16)
    grad_conv = lax.optimization_barrier(grad_conv)
    later = passed_along(grad_conv[: taps - 1], SP, -1)
    own_grad = grad_conv.astype(jnp.float32)
    tap_list = []
    for offset in range(taps):
        tap_list.append(jnp.sum(own_grad * padded_in[offset : offset + rows_here], 0))
    tail = jnp.stack(tap_list + [gain_part], 0)
    tail = tail.reshape(y_size, (taps + 1) // y_size, width_dp)
    tail = [lax.dynamic_index_in_dim(tail, (y_here + k) % y_size, 0, False) for k in range(y_size)]
    tail = sum([shifted(tail[k], "sp_1", k) for k in ahead], tail[0]).astype(jnp.bfloat16)
    tail, weight_part = lax.optimization_barrier((tail, weight_part))
    grad_out_weight = undense(weight_part.astype(jnp.float32).sum(axis=0))
    tail = from_everyone(tail, "sp_0").astype(jnp.float32).sum(axis=0)
    tail = jnp.stack([tail] + [shifted(tail, "sp_1", -k) for k in ahead])
    tail = jnp.concatenate([tail, tail], 0)
    tail = lax.dynamic_slice_in_dim(tail, (y_size - y_here) % y_size, y_size, 0)
    tail = tail.reshape(taps + 1, width_dp)
    grad_taps, grad_gain = (tail[:taps], tail[taps])

    padded_grad = jnp.concatenate([grad_conv, later], 0).astype(jnp.float32)
    grad_mixed = jnp.zeros((rows_here, width_dp), jnp.float32)
    for offset in range(taps):
        back = taps - 1 - offset
        grad_mixed = grad_mixed + conv_taps[offset][None, :] * padded_grad[back : back + rows_here]
    grad_rows = lax.optimization_barrier(grad_mixed.astype(jnp.bfloat16)).astype(jnp.float32)
    grad_val = (grad_rows * sigma_gate).astype(jnp.bfloat16)
    grad_gate = (
        grad_rows * val_input.astype(jnp.float32) * sigma_gate * (1.0 - sigma_gate)
    ).astype(jnp.bfloat16)
    return (grad_val, grad_gate, grad_out_weight, grad_taps, grad_gain)


def solution(mesh):
    split = Mesh(mesh.devices.reshape(16, 4, mesh.shape["dp"]), ("sp_0", "sp_1", "dp"))
    in_specs = (P(SP, "dp"), P(SP, "dp"), P(SP, None), P(SP, "dp"), P(None, "dp"), P("dp"))
    out_specs = (P(SP, "dp"), P(SP, "dp"), P(SP, "dp"), P(None, "dp"), P("dp"))

    return jax.shard_map(
        per_device, mesh=split, in_specs=in_specs, out_specs=out_specs, check_vma=False
    )
```

```python
import jax
import jax.numpy as jnp
from jax import lax
from jax.sharding import Mesh
from jax.sharding import PartitionSpec as P

SP = ("sp_0", "sp_1")


norm_floor = 0.25


def passed_along(value, axis, steps):
    count = lax.axis_size(axis)
    first, last = (max(0, -steps), min(count, count - steps))
    return lax.ppermute(value, axis, [(source, source + steps) for source in range(first, last)])


def exchange(blocks, axis):
    return lax.all_to_all(blocks, axis, split_axis=0, concat_axis=0, tiled=True)


def from_everyone(array, axis):
    return exchange(jnp.broadcast_to(array, (lax.axis_size(axis), *array.shape)), axis)


def swapped(value, axis, k):
    return lax.ppermute(value, axis, [(i, i ^ k) for i in range(lax.axis_size(axis))])


def pairs_total(value, axis):
    k = 1
    while k < lax.axis_size(axis):
        value = value + swapped(value, axis, k)
        k *= 2
    return value


def reordered(blocks, index):
    k = 1
    while k < len(blocks):
        swap = (index & k) != 0
        blocks = [jnp.where(swap, blocks[j ^ k], blocks[j]) for j in range(len(blocks))]
        k *= 2
    return blocks


def dense(blocks):
    half = blocks.shape[-2] // 2
    rest = jnp.concatenate([blocks[..., :half, 128:], blocks[..., half:, 128:]], -1)
    return jnp.concatenate([blocks[..., :128], rest], -2)


def undense(blocks):
    rows = blocks.shape[-2] * 2 // 3
    rest = blocks[..., rows:, :]
    rest = jnp.concatenate([rest[..., :64], rest[..., 64:]], -2)
    return jnp.concatenate([blocks[..., :rows, :], rest], -1)


def per_device(val_input, gate_input, cotangent, out_weight, conv_taps, norm_gain):
    rows_here = val_input.shape[0]
    width_dp = val_input.shape[1]
    taps = conv_taps.shape[0]
    channels = width_dp * lax.axis_size("dp")
    z_size, y_size = (lax.axis_size("sp_0"), lax.axis_size("sp_1"))
    d_rows = out_weight.shape[0]

    y_here = lax.axis_index("sp_1")
    others = range(1, y_size)

    weight = from_everyone(dense(out_weight), "sp_0")
    blocks = cotangent.reshape(rows_here, z_size, y_size, d_rows).transpose(2, 0, 1, 3)
    blocks = blocks.reshape(y_size, rows_here, z_size * d_rows)
    blocks = [lax.dynamic_index_in_dim(blocks, y_here ^ k, 0, False) for k in range(y_size)]
    columns = [blocks[0]] + [swapped(blocks[k], "sp_1", k) for k in others]

    sigma_gate = jax.nn.sigmoid(gate_input.astype(jnp.float32))
    mixed_in = (val_input.astype(jnp.float32) * sigma_gate).astype(jnp.bfloat16)
    earlier = passed_along(mixed_in[rows_here - (taps - 1) :], SP, 1)
    padded_in = jnp.concatenate([earlier, lax.optimization_barrier(mixed_in)], 0).astype(
        jnp.float32
    )
    conv_out = jnp.zeros((rows_here, width_dp), jnp.float32)
    for offset in range(taps):
        conv_out = conv_out + conv_taps[offset][None, :] * padded_in[offset : offset + rows_here]
    conv_rows = lax.optimization_barrier(conv_out.astype(jnp.bfloat16)).astype(jnp.float32)
    row_sums = jnp.stack([jnp.sum(conv_rows, 1), jnp.sum(conv_rows * conv_rows, 1)])
    row_sums = pairs_total(row_sums, "dp")
    row_mean = row_sums[0][:, None] / channels
    row_var = row_sums[1][:, None] / channels - row_mean * row_mean
    inv_scale = lax.rsqrt(row_var + norm_floor)
    normed = (conv_rows - row_mean) * inv_scale
    act = normed * norm_gain[None, :]
    sigma_act = jax.nn.sigmoid(act)
    swished = (act * sigma_act).astype(jnp.bfloat16)

    weight, swished = lax.optimization_barrier((weight, swished))
    weight = undense(weight).reshape(z_size * d_rows, width_dp)
    mix_parts = [
        jnp.dot(c, weight, preferred_element_type=jnp.float32).astype(jnp.bfloat16) for c in columns
    ]
    sent = [jnp.concatenate([part, swished], 1) for part in reordered(mix_parts, y_here)]
    received = exchange(jnp.stack(sent), "sp_1")
    grad_mix = received[:, :, :width_dp].astype(jnp.float32).sum(axis=0)
    swished_y = reordered([received[i, :, width_dp:] for i in range(y_size)], y_here)
    weight_part = lax.dot_general(
        jnp.concatenate(columns, 0),
        jnp.concatenate(swished_y, 0),
        (((0,), (0,)), ((), ())),
        preferred_element_type=jnp.float32,
    )
    weight_part = dense(weight_part.astype(jnp.bfloat16).reshape(z_size, d_rows, width_dp))

    grad_act = grad_mix * sigma_act * (1.0 + act * (1.0 - sigma_act))
    gain_part = jnp.sum(grad_act * normed, 0)
    grad_norm = grad_act * norm_gain[None, :]
    norm_sums = jnp.stack([jnp.sum(grad_norm, 1), jnp.sum(grad_norm * normed, 1)])
    norm_sums = from_everyone(norm_sums, "dp").sum(axis=0)
    first_sum = norm_sums[0][:, None] / channels
    second_sum = norm_sums[1][:, None] / channels
    grad_conv = (inv_scale * (grad_norm - first_sum - normed * second_sum)).astype(jnp.bfloat16)
    grad_conv = lax.optimization_barrier(grad_conv)
    later = passed_along(grad_conv[: taps - 1], SP, -1)
    own_grad = grad_conv.astype(jnp.float32)
    tap_list = []
    for offset in range(taps):
        tap_list.append(jnp.sum(own_grad * padded_in[offset : offset + rows_here], 0))
    tail = dense(jnp.stack(tap_list + [gain_part], 0))
    tail = from_everyone(tail, "sp_1").sum(axis=0).astype(jnp.bfloat16)
    tail = jnp.broadcast_to(tail, (z_size, *tail.shape))
    sums = exchange(jnp.concatenate([weight_part, tail], 1), "sp_0")
    sums = sums.astype(jnp.float32).sum(axis=0)
    grad_out_weight = undense(sums[: weight_part.shape[1]])
    tail = undense(sums[weight_part.shape[1] :])
    grad_taps, grad_gain = (tail[:taps], tail[taps])

    padded_grad = jnp.concatenate([grad_conv, later], 0).astype(jnp.float32)
    grad_mixed = jnp.zeros((rows_here, width_dp), jnp.float32)
    for offset in range(taps):
        back = taps - 1 - offset
        grad_mixed = grad_mixed + conv_taps[offset][None, :] * padded_grad[back : back + rows_here]
    grad_rows = lax.optimization_barrier(grad_mixed.astype(jnp.bfloat16)).astype(jnp.float32)
    grad_val = (grad_rows * sigma_gate).astype(jnp.bfloat16)
    grad_gate = (
        grad_rows * val_input.astype(jnp.float32) * sigma_gate * (1.0 - sigma_gate)
    ).astype(jnp.bfloat16)
    return (grad_val, grad_gate, grad_out_weight, grad_taps, grad_gain)


def solution(mesh):
    split = Mesh(mesh.devices.reshape(16, 4, mesh.shape["dp"]), ("sp_0", "sp_1", "dp"))
    in_specs = (P(SP, "dp"), P(SP, "dp"), P(SP, None), P(SP, "dp"), P(None, "dp"), P("dp"))
    out_specs = (P(SP, "dp"), P(SP, "dp"), P(SP, "dp"), P(None, "dp"), P("dp"))
    return jax.shard_map(
        per_device, mesh=split, in_specs=in_specs, out_specs=out_specs, check_vma=False
    )
```

```python
import jax
import jax.numpy as jnp
from jax import lax
from jax.sharding import Mesh
from jax.sharding import PartitionSpec as P


SP = ("z_far", "z_near", "sp_1")
Z = ("z_far", "z_near")


norm_floor = 0.25


def passed_along(value, axis, steps):
    count = lax.axis_size(axis)
    first, last = (max(0, -steps), min(count, count - steps))
    return lax.ppermute(value, axis, [(source, source + steps) for source in range(first, last)])


def exchange(blocks, axis):
    return lax.all_to_all(blocks, axis, split_axis=0, concat_axis=0, tiled=True)


def from_everyone(array, axis):
    return exchange(jnp.broadcast_to(array, (lax.axis_size(axis), *array.shape)), axis)


def swapped(value, axis, k):
    return lax.ppermute(value, axis, [(i, i ^ k) for i in range(lax.axis_size(axis))])


def reordered(blocks, index):
    k = 1
    while k < len(blocks):
        swap = (index & k) != 0
        blocks = [jnp.where(swap, blocks[j ^ k], blocks[j]) for j in range(len(blocks))]
        k *= 2
    return blocks


def dense(blocks):
    half = blocks.shape[-2] // 2
    rest = jnp.concatenate([blocks[..., :half, 128:], blocks[..., half:, 128:]], -1)
    return jnp.concatenate([blocks[..., :128], rest], -2)


def undense(blocks):
    rows = blocks.shape[-2] * 2 // 3
    rest = blocks[..., rows:, :]
    rest = jnp.concatenate([rest[..., :64], rest[..., 64:]], -2)
    return jnp.concatenate([blocks[..., :rows, :], rest], -1)


def per_device(val_input, gate_input, cotangent, out_weight, conv_taps, norm_gain):
    rows_here = val_input.shape[0]
    width_dp = val_input.shape[1]
    taps = conv_taps.shape[0]
    channels = width_dp * lax.axis_size("dp")
    z_size, y_size = (lax.axis_size(Z), lax.axis_size("sp_1"))
    d_rows = out_weight.shape[0]

    y_here = lax.axis_index("sp_1")
    others = range(1, y_size)

    weight = from_everyone(dense(out_weight), Z)
    blocks = cotangent.reshape(rows_here, z_size, y_size, d_rows).transpose(2, 0, 1, 3)
    blocks = blocks.reshape(y_size, rows_here, z_size * d_rows)
    blocks = [lax.dynamic_index_in_dim(blocks, y_here ^ k, 0, False) for k in range(y_size)]
    columns = [blocks[0]] + [swapped(blocks[k], "sp_1", k) for k in others]

    sigma_gate = jax.nn.sigmoid(gate_input.astype(jnp.float32))
    mixed_in = (val_input.astype(jnp.float32) * sigma_gate).astype(jnp.bfloat16)
    earlier = passed_along(mixed_in[rows_here - (taps - 1) :], SP, 1)
    padded_in = jnp.concatenate([earlier, lax.optimization_barrier(mixed_in)], 0).astype(
        jnp.float32
    )
    conv_out = jnp.zeros((rows_here, width_dp), jnp.float32)
    for offset in range(taps):
        conv_out = conv_out + conv_taps[offset][None, :] * padded_in[offset : offset + rows_here]
    conv_rows = lax.optimization_barrier(conv_out.astype(jnp.bfloat16)).astype(jnp.float32)
    row_sums = jnp.stack([jnp.sum(conv_rows, 1), jnp.sum(conv_rows * conv_rows, 1)])
    weight, row_sums = lax.optimization_barrier((weight, row_sums))
    row_sums = from_everyone(row_sums, "dp").sum(axis=0)
    row_mean = row_sums[0][:, None] / channels
    row_var = row_sums[1][:, None] / channels - row_mean * row_mean
    inv_scale = lax.rsqrt(row_var + norm_floor)
    normed = (conv_rows - row_mean) * inv_scale
    act = normed * norm_gain[None, :]
    sigma_act = jax.nn.sigmoid(act)
    swished = (act * sigma_act).astype(jnp.bfloat16)

    weight = undense(weight).reshape(z_size * d_rows, width_dp)
    mix_parts = [
        jnp.dot(c, weight, preferred_element_type=jnp.float32).astype(jnp.bfloat16) for c in columns
    ]
    sent = [jnp.concatenate([part, swished], 1) for part in reordered(mix_parts, y_here)]
    received = exchange(jnp.stack(sent), "sp_1")
    grad_mix = received[:, :, :width_dp].astype(jnp.float32).sum(axis=0)
    swished_y = reordered([received[i, :, width_dp:] for i in range(y_size)], y_here)
    weight_part = lax.dot_general(
        jnp.concatenate(columns, 0),
        jnp.concatenate(swished_y, 0),
        (((0,), (0,)), ((), ())),
        preferred_element_type=jnp.float32,
    )
    weight_part = dense(weight_part.astype(jnp.bfloat16).reshape(z_size, d_rows, width_dp))

    grad_act = grad_mix * sigma_act * (1.0 + act * (1.0 - sigma_act))
    gain_part = jnp.sum(grad_act * normed, 0)
    grad_norm = grad_act * norm_gain[None, :]
    norm_sums = jnp.stack([jnp.sum(grad_norm, 1), jnp.sum(grad_norm * normed, 1)])
    norm_sums = from_everyone(norm_sums, "dp").sum(axis=0)
    first_sum = norm_sums[0][:, None] / channels
    second_sum = norm_sums[1][:, None] / channels
    grad_conv = (inv_scale * (grad_norm - first_sum - normed * second_sum)).astype(jnp.bfloat16)
    grad_conv = lax.optimization_barrier(grad_conv)
    later = passed_along(grad_conv[: taps - 1], SP, -1)
    own_grad = grad_conv.astype(jnp.float32)
    tap_list = []
    for offset in range(taps):
        tap_list.append(jnp.sum(own_grad * padded_in[offset : offset + rows_here], 0))
    tail = dense(jnp.stack(tap_list + [gain_part], 0))
    tail = from_everyone(tail, "sp_1").sum(axis=0).astype(jnp.bfloat16)
    near, far = (lax.axis_size("z_near"), lax.axis_size("z_far"))
    part = weight_part.reshape(far, near, -1, weight_part.shape[-1]).transpose(1, 0, 2, 3)
    part = part.reshape(near, -1, weight_part.shape[-1])
    sums = jnp.concatenate([part, jnp.broadcast_to(tail, (near, *tail.shape))], 1)
    sums = exchange(sums, "z_near").astype(jnp.float32).sum(axis=0).astype(jnp.bfloat16)
    tail = sums[part.shape[1] :]
    part = sums[: part.shape[1]].reshape(far, -1, weight_part.shape[-1])
    sums = jnp.concatenate([part, jnp.broadcast_to(tail, (far, *tail.shape))], 1)
    sums = exchange(sums, "z_far").astype(jnp.float32).sum(axis=0)
    grad_out_weight = undense(sums[: part.shape[1]])
    tail = undense(sums[part.shape[1] :])
    grad_taps, grad_gain = (tail[:taps], tail[taps])

    padded_grad = jnp.concatenate([grad_conv, later], 0).astype(jnp.float32)
    grad_mixed = jnp.zeros((rows_here, width_dp), jnp.float32)
    for offset in range(taps):
        back = taps - 1 - offset
        grad_mixed = grad_mixed + conv_taps[offset][None, :] * padded_grad[back : back + rows_here]
    grad_rows = lax.optimization_barrier(grad_mixed.astype(jnp.bfloat16)).astype(jnp.float32)
    grad_val = (grad_rows * sigma_gate).astype(jnp.bfloat16)
    grad_gate = (
        grad_rows * val_input.astype(jnp.float32) * sigma_gate * (1.0 - sigma_gate)
    ).astype(jnp.bfloat16)
    return (grad_val, grad_gate, grad_out_weight, grad_taps, grad_gain)


def solution(mesh):
    split = Mesh(mesh.devices.reshape(4, 4, 4, mesh.shape["dp"]), (*SP, "dp"))
    in_specs = (P(SP, "dp"), P(SP, "dp"), P(SP, None), P(SP, "dp"), P(None, "dp"), P("dp"))
    out_specs = (P(SP, "dp"), P(SP, "dp"), P(SP, "dp"), P(None, "dp"), P("dp"))

    return jax.shard_map(
        per_device, mesh=split, in_specs=in_specs, out_specs=out_specs, check_vma=False
    )
```

```python
import jax
import jax.numpy as jnp
from jax import lax
from jax.experimental.layout import Layout, with_layout_constraint
from jax.sharding import Mesh
from jax.sharding import PartitionSpec as P


SP = ("z_far", "z_near", "sp_1")
Z = ("z_far", "z_near")


norm_floor = 0.25


def passed_along(value, axis, steps):
    count = lax.axis_size(axis)
    first, last = (max(0, -steps), min(count, count - steps))
    return lax.ppermute(value, axis, [(source, source + steps) for source in range(first, last)])


def exchange(blocks, axis):
    return lax.all_to_all(blocks, axis, split_axis=0, concat_axis=0, tiled=True)


def from_everyone(array, axis):
    return exchange(jnp.broadcast_to(array, (lax.axis_size(axis), *array.shape)), axis)


def packed(rows):
    turned = rows.T
    quarter = turned.shape[0] // 4
    return jnp.concatenate([turned[quarter * j : quarter * (j + 1)] for j in range(4)], 1)


def unpacked(block):
    tokens = block.shape[1] // 4
    parts = [block[:, tokens * j : tokens * (j + 1)] for j in range(4)]
    return jnp.concatenate(parts, 0).T


def swapped(value, axis, k):
    return lax.ppermute(value, axis, [(i, i ^ k) for i in range(lax.axis_size(axis))])


def reordered(blocks, index):
    k = 1
    while k < len(blocks):
        swap = (index & k) != 0
        blocks = [jnp.where(swap, blocks[j ^ k], blocks[j]) for j in range(len(blocks))]
        k *= 2
    return blocks


def tokens_major(array):
    return with_layout_constraint(array, Layout(major_to_minor=(0, 1)))


def dense(blocks):
    half = blocks.shape[-2] // 2
    rest = jnp.concatenate([blocks[..., :half, 128:], blocks[..., half:, 128:]], -1)
    return jnp.concatenate([blocks[..., :128], rest], -2)


def undense(blocks):
    rows = blocks.shape[-2] * 2 // 3
    rest = blocks[..., rows:, :]
    rest = jnp.concatenate([rest[..., :64], rest[..., 64:]], -2)
    return jnp.concatenate([blocks[..., :rows, :], rest], -1)


def per_device(val_input, gate_input, cotangent, out_weight, conv_taps, norm_gain):
    rows_here = val_input.shape[0]
    width_dp = val_input.shape[1]
    taps = conv_taps.shape[0]
    channels = width_dp * lax.axis_size("dp")
    z_size, y_size = (lax.axis_size(Z), lax.axis_size("sp_1"))
    d_rows = out_weight.shape[0]

    y_here = lax.axis_index("sp_1")
    others = range(1, y_size)

    weight = from_everyone(dense(out_weight), Z)
    blocks = cotangent.reshape(rows_here, z_size, y_size, d_rows).transpose(2, 0, 1, 3)
    blocks = blocks.reshape(y_size, rows_here, z_size * d_rows)
    blocks = [lax.dynamic_index_in_dim(blocks, y_here ^ k, 0, False) for k in range(y_size)]
    columns = [blocks[0]] + [swapped(blocks[k], "sp_1", k) for k in others]

    sigma_gate = jax.nn.sigmoid(gate_input.astype(jnp.float32))
    mixed_in = (val_input.astype(jnp.float32) * sigma_gate).astype(jnp.bfloat16)
    earlier = passed_along(packed(mixed_in[rows_here - (taps + 1) :]), SP, 1)
    earlier = unpacked(earlier)[2:]
    padded_in = jnp.concatenate([earlier, lax.optimization_barrier(mixed_in)], 0).astype(
        jnp.float32
    )
    conv_out = jnp.zeros((rows_here, width_dp), jnp.float32)
    for offset in range(taps):
        conv_out = conv_out + conv_taps[offset][None, :] * padded_in[offset : offset + rows_here]
    conv_rows = lax.optimization_barrier(conv_out.astype(jnp.bfloat16)).astype(jnp.float32)
    row_sums = jnp.stack([jnp.sum(conv_rows, 1), jnp.sum(conv_rows * conv_rows, 1)])
    weight, row_sums = lax.optimization_barrier((weight, row_sums))
    row_sums = from_everyone(row_sums, "dp").sum(axis=0)
    row_mean = row_sums[0][:, None] / channels
    row_var = row_sums[1][:, None] / channels - row_mean * row_mean
    inv_scale = lax.rsqrt(row_var + norm_floor)
    normed = (conv_rows - row_mean) * inv_scale
    act = normed * norm_gain[None, :]
    sigma_act = jax.nn.sigmoid(act)
    swished = (act * sigma_act).astype(jnp.bfloat16)

    weight = undense(weight).reshape(z_size * d_rows, width_dp)
    mix_parts = [
        jnp.dot(c, weight, preferred_element_type=jnp.float32).astype(jnp.bfloat16) for c in columns
    ]
    sent = [jnp.concatenate([part, swished], 1) for part in reordered(mix_parts, y_here)]
    received = exchange(jnp.stack(sent), "sp_1")
    grad_mix = received[:, :, :width_dp].astype(jnp.float32).sum(axis=0)
    swished_y = reordered([received[i, :, width_dp:] for i in range(y_size)], y_here)
    weight_part = lax.dot_general(
        jnp.concatenate(columns, 0),
        jnp.concatenate(swished_y, 0),
        (((0,), (0,)), ((), ())),
        preferred_element_type=jnp.float32,
    )
    weight_part = dense(weight_part.astype(jnp.bfloat16).reshape(z_size, d_rows, width_dp))
    near, far = (lax.axis_size("z_near"), lax.axis_size("z_far"))
    near_here = lax.axis_index("z_near")
    part = weight_part.reshape(far, near, -1, weight_part.shape[-1])
    part = [lax.dynamic_index_in_dim(part, near_here ^ k, 1, False) for k in range(near)]
    arrived = [swapped(part[near - 1], "z_near", near - 1)]
    arrived += [swapped(part[k], "z_near", k) for k in range(1, near - 1)]

    grad_act = grad_mix * sigma_act * (1.0 + act * (1.0 - sigma_act))
    gain_part = jnp.sum(grad_act * normed, 0)
    grad_norm = grad_act * norm_gain[None, :]
    norm_sums = jnp.stack([jnp.sum(grad_norm, 1), jnp.sum(grad_norm * normed, 1)])
    norm_sums = from_everyone(norm_sums, "dp").sum(axis=0)
    first_sum = norm_sums[0][:, None] / channels
    second_sum = norm_sums[1][:, None] / channels
    grad_conv = (inv_scale * (grad_norm - first_sum - normed * second_sum)).astype(jnp.bfloat16)
    grad_conv = lax.optimization_barrier(grad_conv)
    later = passed_along(grad_conv[: taps - 1], SP, -1)
    own_grad = tokens_major(grad_conv).astype(jnp.float32)
    tap_rows = tokens_major(padded_in.astype(jnp.bfloat16)).astype(jnp.float32)
    tap_list = []
    for offset in range(taps):
        tap_list.append(jnp.sum(own_grad * tap_rows[offset : offset + rows_here], 0))
    tail = dense(jnp.stack(tap_list + [gain_part], 0)).astype(jnp.bfloat16)
    tail = from_everyone(tail, ("z_near", "sp_1"))
    tail = tail.astype(jnp.float32).sum(axis=0).astype(jnp.bfloat16)
    part = sum([p.astype(jnp.float32) for p in arrived], part[0].astype(jnp.float32))
    part = part.astype(jnp.bfloat16)
    sums = jnp.concatenate([part, jnp.broadcast_to(tail, (far, *tail.shape))], 1)
    sums = exchange(sums, "z_far")
    sums = sums.astype(jnp.float32).sum(axis=0)
    grad_out_weight = undense(sums[: part.shape[1]])
    tail = undense(sums[part.shape[1] :])
    grad_taps, grad_gain = (tail[:taps], tail[taps])

    padded_grad = jnp.concatenate([grad_conv, later], 0).astype(jnp.float32)
    grad_mixed = jnp.zeros((rows_here, width_dp), jnp.float32)
    for offset in range(taps):
        back = taps - 1 - offset
        grad_mixed = grad_mixed + conv_taps[offset][None, :] * padded_grad[back : back + rows_here]
    grad_rows = lax.optimization_barrier(grad_mixed.astype(jnp.bfloat16)).astype(jnp.float32)
    grad_val = (grad_rows * sigma_gate).astype(jnp.bfloat16)
    grad_gate = (
        grad_rows * val_input.astype(jnp.float32) * sigma_gate * (1.0 - sigma_gate)
    ).astype(jnp.bfloat16)
    return (grad_val, grad_gate, grad_out_weight, grad_taps, grad_gain)


def solution(mesh):
    split = Mesh(mesh.devices.reshape(4, 4, 4, mesh.shape["dp"]), (*SP, "dp"))
    in_specs = (P(SP, "dp"), P(SP, "dp"), P(SP, None), P(SP, "dp"), P(None, "dp"), P("dp"))
    out_specs = (P(SP, "dp"), P(SP, "dp"), P(SP, "dp"), P(None, "dp"), P("dp"))

    return jax.shard_map(
        per_device, mesh=split, in_specs=in_specs, out_specs=out_specs, check_vma=False
    )
```

```python
import jax
import jax.numpy as jnp
from jax import lax
from jax.experimental.layout import Layout, with_layout_constraint
from jax.sharding import Mesh
from jax.sharding import PartitionSpec as P


SP = ("z_far", "z_near", "sp_1")
Z = ("z_far", "z_near")


norm_floor = 0.25


def passed_along(value, axis, steps):
    count = lax.axis_size(axis)
    first, last = (max(0, -steps), min(count, count - steps))
    return lax.ppermute(value, axis, [(source, source + steps) for source in range(first, last)])


def exchange(blocks, axis):
    return lax.all_to_all(blocks, axis, split_axis=0, concat_axis=0, tiled=True)


def from_everyone(array, axis):
    return exchange(jnp.broadcast_to(array, (lax.axis_size(axis), *array.shape)), axis)


def packed(rows):
    turned = rows.T
    quarter = turned.shape[0] // 4
    return jnp.concatenate([turned[quarter * j : quarter * (j + 1)] for j in range(4)], 1)


def unpacked(block):
    tokens = block.shape[1] // 4
    parts = [block[:, tokens * j : tokens * (j + 1)] for j in range(4)]
    return jnp.concatenate(parts, 0).T


def swapped(value, axis, k):
    return lax.ppermute(value, axis, [(i, i ^ k) for i in range(lax.axis_size(axis))])


def reordered(blocks, index):
    k = 1
    while k < len(blocks):
        swap = (index & k) != 0
        blocks = [jnp.where(swap, blocks[j ^ k], blocks[j]) for j in range(len(blocks))]
        k *= 2
    return blocks


def tokens_major(array):
    return with_layout_constraint(array, Layout(major_to_minor=(0, 1)))


def dense(blocks):
    half = blocks.shape[-2] // 2
    rest = jnp.concatenate([blocks[..., :half, 128:], blocks[..., half:, 128:]], -1)
    return jnp.concatenate([blocks[..., :128], rest], -2)


def undense(blocks):
    rows = blocks.shape[-2] * 2 // 3
    rest = blocks[..., rows:, :]
    rest = jnp.concatenate([rest[..., :64], rest[..., 64:]], -2)
    return jnp.concatenate([blocks[..., :rows, :], rest], -1)


def per_device(val_input, gate_input, cotangent, out_weight, conv_taps, norm_gain):
    rows_here = val_input.shape[0]
    width_dp = val_input.shape[1]
    taps = conv_taps.shape[0]
    channels = width_dp * lax.axis_size("dp")
    z_size, y_size = (lax.axis_size(Z), lax.axis_size("sp_1"))
    d_rows = out_weight.shape[0]

    y_here = lax.axis_index("sp_1")
    others = range(1, y_size)

    weight = with_layout_constraint(out_weight, Layout(major_to_minor=(1, 0)))
    weight = from_everyone(dense(lax.optimization_barrier(weight)), Z)
    blocks = cotangent.reshape(rows_here, z_size, y_size, d_rows).transpose(2, 0, 1, 3)
    blocks = blocks.reshape(y_size, rows_here, z_size * d_rows)
    blocks = [lax.dynamic_index_in_dim(blocks, y_here ^ k, 0, False) for k in range(y_size)]
    columns = [blocks[0]] + [swapped(blocks[k], "sp_1", k) for k in others]

    sigma_gate = jax.nn.sigmoid(gate_input.astype(jnp.float32))
    mixed_in = (val_input.astype(jnp.float32) * sigma_gate).astype(jnp.bfloat16)
    earlier = passed_along(packed(mixed_in[rows_here - (taps + 1) :]), SP, 1)
    earlier = unpacked(earlier)[2:]
    padded_in = jnp.concatenate([earlier, lax.optimization_barrier(mixed_in)], 0).astype(
        jnp.float32
    )
    conv_out = jnp.zeros((rows_here, width_dp), jnp.float32)
    for offset in range(taps):
        conv_out = conv_out + conv_taps[offset][None, :] * padded_in[offset : offset + rows_here]
    conv_rows = lax.optimization_barrier(conv_out.astype(jnp.bfloat16)).astype(jnp.float32)
    row_sums = jnp.stack([jnp.sum(conv_rows, 1), jnp.sum(conv_rows * conv_rows, 1)])
    weight, row_sums = lax.optimization_barrier((weight, row_sums))
    row_sums = from_everyone(row_sums, "dp").sum(axis=0)
    row_mean = row_sums[0][:, None] / channels
    row_var = row_sums[1][:, None] / channels - row_mean * row_mean
    inv_scale = lax.rsqrt(row_var + norm_floor)
    normed = (conv_rows - row_mean) * inv_scale
    act = normed * norm_gain[None, :]
    sigma_act = jax.nn.sigmoid(act)
    swished = (act * sigma_act).astype(jnp.bfloat16)

    weight = undense(weight).reshape(z_size * d_rows, width_dp)
    mix_parts = [
        jnp.dot(c, weight, preferred_element_type=jnp.float32).astype(jnp.bfloat16) for c in columns
    ]
    sent = [jnp.concatenate([part, swished], 1) for part in reordered(mix_parts, y_here)]
    near_here = lax.axis_index("z_near").astype(jnp.uint32)
    near_at = [near_here ^ jnp.uint32(k) for k in range(lax.axis_size("z_near"))]
    sent, near_at = lax.optimization_barrier((jnp.stack(sent), near_at))
    received = exchange(sent, "sp_1")
    grad_mix = received[:, :, :width_dp].astype(jnp.float32).sum(axis=0)
    swished_y = reordered([received[i, :, width_dp:] for i in range(y_size)], y_here)
    weight_part = lax.dot_general(
        jnp.concatenate(columns, 0),
        jnp.concatenate(swished_y, 0),
        (((0,), (0,)), ((), ())),
        preferred_element_type=jnp.float32,
    )
    weight_part = dense(weight_part.astype(jnp.bfloat16).reshape(z_size, d_rows, width_dp))
    near, far = (lax.axis_size("z_near"), lax.axis_size("z_far"))
    part = weight_part.reshape(far, near, -1, weight_part.shape[-1])
    part = [lax.dynamic_index_in_dim(part, near_at[k], 1, False) for k in range(near)]
    arrived = [swapped(part[near - 1], "z_near", near - 1)]
    arrived += [swapped(part[k], "z_near", k) for k in range(1, near - 1)]

    grad_act = grad_mix * sigma_act * (1.0 + act * (1.0 - sigma_act))
    gain_part = jnp.sum(grad_act * normed, 0)
    grad_norm = grad_act * norm_gain[None, :]
    norm_sums = jnp.stack([jnp.sum(grad_norm, 1), jnp.sum(grad_norm * normed, 1)])
    norm_sums = from_everyone(norm_sums, "dp").sum(axis=0)
    first_sum = norm_sums[0][:, None] / channels
    second_sum = norm_sums[1][:, None] / channels
    grad_conv = (inv_scale * (grad_norm - first_sum - normed * second_sum)).astype(jnp.bfloat16)
    grad_conv = lax.optimization_barrier(grad_conv)
    later = passed_along(grad_conv[: taps - 1], SP, -1)
    own_grad = tokens_major(grad_conv).astype(jnp.float32)
    tap_rows = tokens_major(padded_in.astype(jnp.bfloat16)).astype(jnp.float32)
    tap_list = []
    for offset in range(taps):
        tap_list.append(jnp.sum(own_grad * tap_rows[offset : offset + rows_here], 0))
    tail = dense(jnp.stack(tap_list + [gain_part], 0)).astype(jnp.bfloat16)
    tail = from_everyone(tail, ("z_near", "sp_1"))
    tail = tail.astype(jnp.float32).sum(axis=0).astype(jnp.bfloat16)
    part = sum([p.astype(jnp.float32) for p in arrived], part[0].astype(jnp.float32))
    part = part.astype(jnp.bfloat16)
    sums = jnp.concatenate([part, jnp.broadcast_to(tail, (far, *tail.shape))], 1)
    sums = exchange(sums, "z_far")
    sums = sums.astype(jnp.float32).sum(axis=0)
    grad_out_weight = undense(sums[: part.shape[1]])
    tail = undense(sums[part.shape[1] :])
    grad_taps, grad_gain = (tail[:taps], tail[taps])

    padded_grad = jnp.concatenate([grad_conv, later], 0).astype(jnp.float32)
    grad_mixed = jnp.zeros((rows_here, width_dp), jnp.float32)
    for offset in range(taps):
        back = taps - 1 - offset
        grad_mixed = grad_mixed + conv_taps[offset][None, :] * padded_grad[back : back + rows_here]
    grad_rows = lax.optimization_barrier(grad_mixed.astype(jnp.bfloat16)).astype(jnp.float32)
    grad_val = (grad_rows * sigma_gate).astype(jnp.bfloat16)
    grad_gate = (
        grad_rows * val_input.astype(jnp.float32) * sigma_gate * (1.0 - sigma_gate)
    ).astype(jnp.bfloat16)
    return (grad_val, grad_gate, grad_out_weight, grad_taps, grad_gain)


def solution(mesh):
    split = Mesh(mesh.devices.reshape(4, 4, 4, mesh.shape["dp"]), (*SP, "dp"))
    in_specs = (P(SP, "dp"), P(SP, "dp"), P(SP, None), P(SP, "dp"), P(None, "dp"), P("dp"))
    out_specs = (P(SP, "dp"), P(SP, "dp"), P(SP, "dp"), P(None, "dp"), P("dp"))

    return jax.shard_map(
        per_device, mesh=split, in_specs=in_specs, out_specs=out_specs, check_vma=False
    )
```
